128 devices in a mesh: sp: 64 (over z, y, x), tp: 2 (over core).
Axes of the slice: x: 4, y: 4, z: 4, core: 2. Of those that a mesh axis runs over, the one named last changes fastest.
Arguments:
- input_activity: bfloat16 [8, 4096, 1024], P(None, ('sp', 'tp')), may hold values from -6 to 6
- norm_gain: bfloat16 [1024], replicated, may hold values from 0.75 to 1.25
- w_query: bfloat16 [1024, 256], P(None, 'tp'), may hold values from -0.1875 to 0.1875
- w_key: bfloat16 [1024, 256], P(None, 'tp'), may hold values from -0.1875 to 0.1875
- w_value: bfloat16 [1024, 512], P(None, 'tp'), may hold values from -0.1875 to 0.1875
- w_gate: bfloat16 [1024, 512], P(None, 'tp'), may hold values from -0.1875 to 0.1875
- head_gain: bfloat16 [4, 128], P('tp'), may hold values from 0.75 to 1.25
- w_out: bfloat16 [512, 1024], P('tp'), may hold values from -0.25 to 0.25
- initial_state: float32 [8, 4, 64, 128], P(None, 'tp'), may hold values from -48 to 48
Outputs:
- output: bfloat16 [8, 4096, 1024], P(None, ('sp', 'tp'))
- closing_memory: float32 [8, 4, 64, 128], P(None, 'tp')
The draws below stay inside these ranges and needn't reach their ends.
All inputs are finite; a program needn't handle non-finite values.
Results may differ from the reference program's by a relative error of at most 0.015.
Values may be sent and summed in bfloat16 or wider, within the bound.
A program may use at most 64 MiB of HBM per device.

```python
import jax
import jax.numpy as jnp
from jax import lax

SEQS = 8
STRETCH = 64
D = 1024
HEADS = 4
DK = 64
DV = 128
SEQ = 4096


def shard_levels(stream_key, dims, split, low, high):
    def one(axis_at, parts):
        steps = jax.random.uniform(jax.random.fold_in(jax.random.fold_in(stream_key, 6), axis_at), (parts,), jnp.float32, low / len(split), high / len(split))
        return jnp.repeat(jnp.exp(steps), dims[axis_at] // parts).reshape((-1,) + (1,) * (len(dims) - axis_at - 1))

    level = one(*split[0])
    for cut in split[1:]:
        level = level * one(*cut)
    return level


def normal_values(key, dims, width, most, split=(), kind=jnp.bfloat16):
    result = width * jax.random.normal(key, dims, jnp.float32)
    if split:
        result = result * shard_levels(key, dims, split, -0.22, 0.18)
    return jnp.clip(result, -most, most).astype(kind)


def setup_inputs(seed: int = 0) -> dict:
    key_of = jax.random.split(jax.random.key(seed), 10)
    return {
        "input_activity": normal_values(key_of[0], (SEQS, SEQ, D), 1.0, 6.0, ((1, 128),)),
        "norm_gain": jnp.clip(1.0 + 0.05 * jax.random.normal(key_of[1], (D,), jnp.float32), 0.75, 1.25).astype(jnp.bfloat16),
        "w_query": normal_values(key_of[2], (D, HEADS * DK), D ** -0.5, 0.1875, ((1, 2),)),
        "w_key": normal_values(key_of[3], (D, HEADS * DK), D ** -0.5, 0.1875, ((1, 2),)),
        "w_value": normal_values(key_of[4], (D, HEADS * DV), D ** -0.5, 0.1875, ((1, 2),)),
        "w_gate": normal_values(key_of[5], (D, HEADS * DV), D ** -0.5, 0.1875, ((1, 2),)),
        "head_gain": jnp.clip(1.0 + 0.05 * jax.random.normal(key_of[6], (HEADS, DV), jnp.float32), 0.75, 1.25).astype(jnp.bfloat16),
        "w_out": normal_values(key_of[7], (HEADS * DV, D), (HEADS * DV) ** -0.5, 0.25, ((0, 2),)),
        "initial_state": normal_values(key_of[8], (SEQS, HEADS, DK, DV), (SEQ ** 0.5 / 8), 48.0, ((1, 2),), jnp.float32),
    }


EPS = 1e-06
ROPE_BASE = 10000.0

def rotate(values_in, places):
    size_last = values_in.shape[-1]
    half = size_last // 2
    freqs = ROPE_BASE ** (-jnp.arange(0, size_last, 2, dtype=jnp.float32) / size_last)
    angle = places[:, None] * freqs[None, :]
    cosine = jnp.cos(angle)[None, :, None, :]
    sine = jnp.sin(angle)[None, :, None, :]
    first = values_in[..., :half]
    second = values_in[..., half:]
    return jnp.concatenate([first * cosine - second * sine, first * sine + second * cosine], axis=-1)

def reference(input_activity, norm_gain, w_query, w_key, w_value, w_gate, head_gain, w_out, initial_state):
    floats = input_activity.astype(jnp.float32)
    scaled_unit = (floats * lax.rsqrt(lax.optimization_barrier(jnp.mean(floats * floats, axis=-1, keepdims=True)) + EPS) * norm_gain.astype(jnp.float32)).astype(jnp.bfloat16)
    flat = scaled_unit.reshape(SEQS * SEQ, D)

    def project(weight):
        return jnp.dot(flat, weight, preferred_element_type=jnp.float32).astype(jnp.bfloat16).reshape(SEQS, SEQ, HEADS, -1)
    queries = project(w_query)
    keys_all = project(w_key)
    values_all = project(w_value)
    gates = project(w_gate)
    places = jnp.arange(SEQ, dtype=jnp.float32)
    rot_query = rotate(queries.astype(jnp.float32), places).astype(jnp.bfloat16)
    rot_key = (rotate(keys_all.astype(jnp.float32), places) * DK ** (-0.5)).astype(jnp.bfloat16)
    log_decay = -(0.25 + 0.25 * jnp.arange(HEADS, dtype=jnp.float32)) / SEQ
    blocks = SEQ // STRETCH

    def split_into_groups(field_in):
        return field_in.reshape(SEQS, blocks, STRETCH, HEADS, field_in.shape[-1]).transpose(0, 1, 3, 2, 4).astype(jnp.float32)
    query_blocks = split_into_groups(rot_query)
    key_blocks = split_into_groups(rot_key)
    value_blocks = split_into_groups(values_all)
    steps_idx = jnp.arange(STRETCH, dtype=jnp.float32)
    start_positions = steps_idx[:, None] - steps_idx[None, :]
    mask = jnp.where(start_positions[None] >= 0, jnp.exp(jnp.maximum(start_positions, 0.0)[None] * log_decay[:, None, None]), 0.0)
    scores = jnp.einsum('snhcd,snhkd->snhck', query_blocks, key_blocks) * mask[None, None]
    scores = scores.astype(jnp.bfloat16).astype(jnp.float32)
    inner = jnp.einsum('snhck,snhke->snhce', scores, value_blocks)
    key_decay = jnp.exp((STRETCH - 1 - steps_idx)[None, :] * log_decay[:, None])
    weighted_key = (key_blocks * key_decay[None, None, :, :, None]).astype(jnp.bfloat16).astype(jnp.float32)
    local_state = jnp.einsum('snhcd,snhce->snhde', weighted_key, value_blocks)
    block_decay = jnp.exp(STRETCH * log_decay)[None, :, None, None]

    def advance(state, segment_slice):
        return (state * block_decay + segment_slice, state)
    closing_memory, incoming = lax.scan(advance, initial_state, jnp.moveaxis(local_state, 1, 0))
    query_decay = jnp.exp((steps_idx + 1.0)[None, :] * log_decay[:, None])
    cross = jnp.einsum('snhcd,nshde->snhce', query_blocks * query_decay[None, None, :, :, None], incoming, precision=lax.Precision.HIGHEST)
    retained = (inner + cross).transpose(0, 1, 3, 2, 4).reshape(SEQS, SEQ, HEADS, DV)
    centre = lax.optimization_barrier(jnp.mean(retained, axis=-1, keepdims=True))
    spread = lax.optimization_barrier(jnp.mean(jnp.square(retained - centre), axis=-1, keepdims=True))
    normalized = (retained - centre) * lax.rsqrt(spread + EPS) * head_gain.astype(jnp.float32)[None, None]
    mixed = (jax.nn.silu(gates.astype(jnp.float32)) * normalized).astype(jnp.bfloat16).reshape(SEQS * SEQ, HEADS * DV)
    output = jnp.dot(mixed, w_out, preferred_element_type=jnp.float32).astype(jnp.bfloat16).reshape(SEQS, SEQ, D)
    return (output, closing_memory)
```

```python
import functools

import jax
import jax.numpy as jnp
import numpy as np
from jax import lax
from jax.experimental import pallas as pl
from jax.experimental.pallas import tpu as pltpu
from jax.sharding import Mesh
from jax.sharding import PartitionSpec as P

SP = ("sp_0", "sp_1", "sp_2")
SP_TP = ("sp_0", "sp_1", "sp_2", "tp")
MESH = pl.DeviceIdType.MESH

EPS = 1e-06
ROPE_BASE = 10000.0

SEQS, HALF, D = 8, 32, 1024
STRETCH = 2 * HALF
BLOCKS = 64
DK, DV = 64, 128
KEYS, VALS = 2 * DK, 2 * DV
TILE = 16
F32, BF16 = jnp.float32, jnp.bfloat16


def tables():
    lane = np.arange(KEYS)
    freqs = ROPE_BASE ** (-2.0 * (lane % 32) / DK)
    sign = np.where(lane % DK < 32, -1.0, 1.0)
    start = (np.arange(BLOCKS) * STRETCH)[:, None] * freqs
    step = np.arange(STRETCH)[:, None] * freqs
    base = np.zeros((BLOCKS, 8, KEYS))
    base[:, 0], base[:, 1], base[:, 2] = np.cos(start), np.sin(start), sign * np.sin(start)
    turn = np.stack([np.cos(step), np.sin(step), sign * np.sin(step)])
    lg = -(0.25 + 0.25 * np.arange(4)) / (BLOCKS * STRETCH)
    pos = np.arange(STRETCH)
    decay = np.zeros((2, 208, KEYS))
    mask = np.zeros((2, 4, STRETCH, 2, STRETCH))
    gap = pos[:, None] - pos[None, :]
    for t in range(2):
        for h in range(2):
            g = lg[2 * t + h]
            decay[t, :64, h * DK : (h + 1) * DK] = np.exp((STRETCH - 1 - pos) * g)[:, None]
            decay[t, 64 + 64 * h : 128 + 64 * h] = np.exp((pos + 1) * g)[:, None]
            decay[t, 192 + 8 * h : 200 + 8 * h] = np.exp(STRETCH * g)
            for s in range(2):
                mask[t, 2 * h + s, :, s] = np.where(gap >= 0, np.exp(np.maximum(gap, 0) * g), 0)
    mask = mask.reshape(2, 4 * STRETCH, 2 * STRETCH)
    return [np.asarray(a, np.float32) for a in (base, turn, decay, mask)]


def dot(a, b):
    return jnp.dot(a, b, preferred_element_type=F32)


def layer(
    x_hbm, gain_hbm, wq_hbm, wk_hbm, wv_hbm, wg_hbm, hg_hbm, wo_hbm, init_hbm,
    base_hbm, turn_hbm, decay_hbm, mask_hbm,
    out_hbm, close_hbm,
    x_own, x_oth, gain, w_in, w_own, w_oth, hgain, init, base, turn, decay, mask,
    normed, cosine, sine, keys, wkeys, values, queries, gate, inner,
    send1, recv1, send2, incoming, csend, closing, mix, mix_oth, out, close,
    load_sem, store_sem, xs_sem, xr_sem, a_send, a_recv, sem2, sem3,
):
    z, y, x, t = (lax.axis_index(a) for a in SP_TP)
    me = (z * 4 + y) * 4 + x

    piece = me // 4
    loads = [
        pltpu.make_async_copy(src, dst, load_sem.at[k])
        for k, (src, dst) in enumerate(
            (
                (x_hbm, x_own),
                (gain_hbm, gain),
                (wk_hbm, w_in.at[:, pl.ds(0, KEYS)]),
                (wv_hbm, w_in.at[:, pl.ds(KEYS, VALS)]),
                (base_hbm.at[me], base),
                (turn_hbm, turn),
                (decay_hbm.at[t], decay),
                (wq_hbm, w_in.at[:, pl.ds(KEYS + VALS, KEYS)]),
                (wg_hbm, w_in.at[:, pl.ds(2 * KEYS + VALS, VALS)]),
                (hg_hbm, hgain),
                (mask_hbm.at[t], mask),
                (init_hbm.at[piece // 2, lax.rem(piece, 2), pl.ds(TILE * lax.rem(me, 4), TILE)], init),
                (wo_hbm, w_own),
            )
        )
    ]
    partner = (z, y, x, 1 - t)
    barrier = pltpu.get_barrier_semaphore()
    for k in (1, 2, 3):
        for there in (
            (lax.rem(z + k, 4), y, x, t),
            (z, lax.rem(y + k, 4), x, t),
            (z, y, lax.rem(x + k, 4), t),
        ):
            pl.semaphore_signal(barrier, inc=1, device_id=there, device_id_type=MESH)
    pl.semaphore_signal(barrier, inc=1, device_id=partner, device_id_type=MESH)
    for copy in loads:
        copy.start()

    loads[0].wait()
    pl.semaphore_wait(barrier, 10)
    swap_x = pltpu.make_async_remote_copy(
        src_ref=x_own, dst_ref=x_oth, send_sem=xs_sem.at[0], recv_sem=xr_sem.at[0],
        device_id=partner, device_id_type=MESH,
    )
    swap_x.start()
    for k in (1, 2, 3):
        pl.semaphore_signal(sem2, inc=1, device_id=(z, lax.rem(y + k, 4), x, t), device_id_type=MESH)

    for k in range(1, 7):
        loads[k].wait()
    cosine[...] = base[0:1, :] * turn[0] - base[1:2, :] * turn[1]
    sine[...] = base[2:3, :] * turn[0] + base[0:1, :] * turn[2]

    lane = lax.broadcasted_iota(jnp.int32, (1, 1, KEYS), 2)
    low = lax.rem(lane, DK) < DK // 2
    gains = gain[...].astype(F32)

    def norm(x_ref):
        def rows(s, carry):
            f = x_ref[s].astype(F32)
            ms = jnp.mean(f * f, axis=-1, keepdims=True)
            normed[pl.ds(pl.multiple_of(s * HALF, HALF), HALF), :] = (
                f * lax.rsqrt(ms + EPS) * gains
            ).astype(BF16)
            return carry

        lax.fori_loop(0, SEQS, rows, 0)

    def rotary(p, row):
        v = p.reshape(SEQS, HALF, KEYS)
        flat = p
        other = jnp.where(
            low, pltpu.roll(flat, KEYS - 32, 1).reshape(v.shape), pltpu.roll(flat, 32, 1).reshape(v.shape)
        )
        return v * cosine[pl.ds(row, HALF), :][None] + other * sine[pl.ds(row, HALF), :][None]

    def keys_values(row):
        p = dot(normed[...], w_in[:, : KEYS + VALS])
        values[:, pl.ds(row, HALF), :] = p[:, KEYS:].astype(BF16).reshape(SEQS, HALF, VALS)
        k = (rotary(p[:, :KEYS].astype(BF16).astype(F32), row) * DK**-0.5).astype(BF16)
        keys[:, pl.ds(row, HALF), :] = k
        wkeys[:, pl.ds(row, HALF), :] = (k.astype(F32) * decay[pl.ds(row, HALF), :][None]).astype(BF16)

    def queries_gates(row):
        p = dot(normed[...], w_in[:, KEYS + VALS :])
        queries[:, pl.ds(row, HALF), :] = rotary(p[:, :KEYS].astype(BF16).astype(F32), row).astype(BF16)
        g = p[:, KEYS:].astype(BF16).astype(F32)
        gate[:, pl.ds(row, HALF), :] = jax.nn.silu(g).reshape(SEQS, HALF, VALS)

    row_own = pl.multiple_of(HALF * t, HALF)
    row_oth = pl.multiple_of(HALF * (1 - t), HALF)
    norm(x_own)
    keys_values(row_own)
    pl.semaphore_wait(sem2, 3)
    for k in (1, 2, 3):
        pl.semaphore_signal(sem3, inc=1, device_id=(lax.rem(z + k, 4), y, x, t), device_id_type=MESH)
    for k in range(7, 13):
        loads[k].wait()
    queries_gates(row_own)
    swap_x.wait()
    swap_w = pltpu.make_async_remote_copy(
        src_ref=w_own, dst_ref=w_oth, send_sem=xs_sem.at[1], recv_sem=xr_sem.at[1],
        device_id=partner, device_id_type=MESH,
    )
    swap_w.start()
    norm(x_oth)
    keys_values(row_oth)

    for s in range(SEQS):
        both = dot(wkeys[s].T, values[s])
        for h in range(2):
            part = both[h * DK : (h + 1) * DK, h * DV : (h + 1) * DV].astype(BF16)
            send1[pl.ds((2 * s + h) * 4, 4)] = part.reshape(4, TILE, DV)
    pl.semaphore_wait(sem3, 3)

    def to_all(source, landing, k_sem):
        def one(k, carry):
            there = lax.rem(me + k, BLOCKS)
            pltpu.make_async_remote_copy(
                src_ref=source(there), dst_ref=landing.at[me],
                send_sem=a_send.at[k_sem], recv_sem=a_recv.at[k_sem],
                device_id=(there // 16, lax.rem(there // 4, 4), lax.rem(there, 4), t),
                device_id_type=MESH,
            ).start()
            return carry

        lax.fori_loop(1, BLOCKS, one, 0)

    def await_all(buffer, sem):
        rest = buffer.at[pl.ds(0, BLOCKS - 1)]
        pltpu.make_async_copy(rest, rest, sem).wait()

    to_all(lambda there: send1.at[there], recv1, 0)
    recv1[me] = send1[me]

    queries_gates(row_oth)
    first = lax.broadcasted_iota(jnp.int32, (1, KEYS), 1) < DK
    for j in range(SEQS // 2):
        q = queries[2 * j : 2 * j + 2].reshape(2 * STRETCH, KEYS)
        zero = jnp.zeros_like(q)
        stacked = jnp.concatenate([jnp.where(first, q, zero), jnp.where(first, zero, q)], axis=0)
        k = keys[2 * j : 2 * j + 2].reshape(2 * STRETCH, KEYS)
        scores = lax.dot_general(stacked, k, (((1,), (1,)), ((), ())), preferred_element_type=F32)
        scores = (scores * mask[...]).astype(BF16)
        v = values[2 * j : 2 * j + 2].reshape(2 * STRETCH, VALS)
        for h in range(2):
            cols = slice(h * DV, (h + 1) * DV)
            got = dot(scores[h * 2 * STRETCH : (h + 1) * 2 * STRETCH], v[:, cols])
            inner[2 * j : 2 * j + 2, :, cols] = got.reshape(2, STRETCH, DV)

    block_decay = decay[pl.ds(pl.multiple_of(192 + 8 * lax.rem(piece, 2), 8), 8), :]
    block_decay = jnp.concatenate([block_decay, block_decay], axis=0)
    await_all(recv1, a_recv.at[0])
    state = init[...]
    for j in range(BLOCKS):
        send2[j] = state.astype(BF16)
        state = state * block_decay + recv1[j].astype(F32)
    csend[...] = state.astype(BF16)
    to_all(lambda there: send2.at[there], incoming, 1)
    to_all(lambda there: csend, closing, 2)
    incoming[me] = send2[me]
    closing[me] = csend[...]
    await_all(incoming, a_recv.at[1])

    gains_h = hgain[...].astype(F32)
    for s in range(SEQS):
        q = queries[s]
        s0 = incoming[pl.ds(8 * s, 4)].reshape(DK, DV)
        s1 = incoming[pl.ds(8 * s + 4, 4)].reshape(DK, DV)
        zero = jnp.zeros_like(s0)
        cross = dot(q, jnp.concatenate(
            [jnp.concatenate([s0, zero], axis=1), jnp.concatenate([zero, s1], axis=1)], axis=0
        ))
        for h in range(2):
            cols = slice(h * DV, (h + 1) * DV)
            kept = inner[s, :, cols] + cross[:, cols] * decay[64 + 64 * h : 128 + 64 * h, :]
            kept = kept - jnp.mean(kept, axis=-1, keepdims=True)
            spread = jnp.mean(kept * kept, axis=-1, keepdims=True)
            m = gate[s, :, cols] * (kept * lax.rsqrt(spread + EPS) * gains_h[h : h + 1, :])
            m = m.astype(BF16)
            mix[0, s, :, cols] = m[:HALF]
            mix[1, s, :, cols] = m[HALF:]
    swap_m = pltpu.make_async_remote_copy(
        src_ref=mix.at[1 - t], dst_ref=mix_oth, send_sem=xs_sem.at[2], recv_sem=xr_sem.at[2],
        device_id=partner, device_id_type=MESH,
    )
    swap_m.start()
    part = dot(mix[t].reshape(SEQS * HALF, VALS), w_own[...])
    swap_w.wait()
    swap_m.wait()
    part = part + dot(mix_oth[...].reshape(SEQS * HALF, VALS), w_oth[...])
    out[...] = part.astype(BF16).reshape(SEQS, HALF, D)
    store = pltpu.make_async_copy(out, out_hbm, store_sem.at[0])
    store.start()
    await_all(closing, a_recv.at[2])
    close[...] = closing[...].astype(F32).reshape(SEQS, 2, DK, DV)
    store_c = pltpu.make_async_copy(close, close_hbm, store_sem.at[1])
    store_c.start()
    await_all(send1, a_send.at[0])
    await_all(send2, a_send.at[1])
    await_all(closing, a_send.at[2])
    store.wait()
    store_c.wait()


def per_device(x, norm_gain, w_query, w_key, w_value, w_gate, head_gain, w_out, initial_state):
    any_space = pl.BlockSpec(memory_space=pl.ANY)
    vmem = pltpu.VMEM
    dma = pltpu.SemaphoreType.DMA
    rows = (SEQS, STRETCH)
    args = (
        x, norm_gain.reshape(1, D), w_query, w_key, w_value, w_gate, head_gain, w_out, initial_state,
        *[jnp.asarray(a) for a in tables()],
    )
    return pl.pallas_call(
        layer,
        out_shape=(
            jax.ShapeDtypeStruct(x.shape, BF16),
            jax.ShapeDtypeStruct(initial_state.shape, F32),
        ),
        in_specs=[any_space] * len(args),
        out_specs=(any_space, any_space),
        scratch_shapes=[
            vmem((SEQS, HALF, D), BF16),
            vmem((SEQS, HALF, D), BF16),
            vmem((1, D), BF16),
            vmem((D, 2 * (KEYS + VALS)), BF16),
            vmem((VALS, D), BF16),
            vmem((VALS, D), BF16),
            vmem((2, DV), BF16),
            vmem((TILE, DV), F32),
            vmem((8, KEYS), F32),
            vmem((3, STRETCH, KEYS), F32),
            vmem((208, KEYS), F32),
            vmem((4 * STRETCH, 2 * STRETCH), F32),
            vmem((SEQS * HALF, D), BF16),
            vmem((STRETCH, KEYS), F32),
            vmem((STRETCH, KEYS), F32),
            vmem(rows + (KEYS,), BF16),
            vmem(rows + (KEYS,), BF16),
            vmem(rows + (VALS,), BF16),
            vmem(rows + (KEYS,), BF16),
            vmem(rows + (VALS,), F32),
            vmem(rows + (VALS,), F32),
            vmem((BLOCKS, TILE, DV), BF16),
            vmem((BLOCKS, TILE, DV), BF16),
            vmem((BLOCKS, TILE, DV), BF16),
            vmem((BLOCKS, TILE, DV), BF16),
            vmem((TILE, DV), BF16),
            vmem((BLOCKS, TILE, DV), BF16),
            vmem((2, SEQS, HALF, VALS), BF16),
            vmem((SEQS, HALF, VALS), BF16),
            vmem((SEQS, HALF, D), BF16),
            vmem((SEQS, 2, DK, DV), F32),
            dma((13,)), dma((2,)), dma((3,)), dma((3,)), dma((3,)), dma((3,)),
            pltpu.SemaphoreType.REGULAR, pltpu.SemaphoreType.REGULAR,
        ],
        compiler_params=pltpu.CompilerParams(collective_id=0, has_side_effects=True),
    )(*args)


def solution(mesh):
    split = Mesh(mesh.devices.reshape(4, 4, 4, mesh.shape["tp"]), SP_TP)
    placed = (
        P(None, SP_TP, None),
        P(),
        P(None, "tp"),
        P(None, "tp"),
        P(None, "tp"),
        P(None, "tp"),
        P("tp", None),
        P("tp", None),
        P(None, "tp", None, None),
    )
    return jax.shard_map(
        per_device,
        mesh=split,
        in_specs=placed,
        out_specs=(P(None, SP_TP, None), P(None, "tp", None, None)),
        check_vma=False,
    )
```

```python
import functools

import jax
import jax.numpy as jnp
import numpy as np
from jax import lax
from jax.experimental import pallas as pl
from jax.experimental.pallas import tpu as pltpu
from jax.sharding import Mesh
from jax.sharding import PartitionSpec as P

SP = ("sp_0", "sp_1", "sp_2")
SP_TP = ("sp_0", "sp_1", "sp_2", "tp")
MESH = pl.DeviceIdType.MESH

EPS = 1e-06
ROPE_BASE = 10000.0

SEQS, HALF, D = 8, 32, 1024
STRETCH = 2 * HALF
BLOCKS = 64
DK, DV = 64, 128
KEYS, VALS = 2 * DK, 2 * DV
TILE = 16
F32, BF16 = jnp.float32, jnp.bfloat16
FAR_FIRST = sorted(
    [(a, b, c) for a in range(4) for b in range(4) for c in range(4) if a or b or c],
    key=lambda o: -sum(min(k, 4 - k) for k in o),
)


def tables():
    lane = np.arange(KEYS)
    freqs = ROPE_BASE ** (-2.0 * (lane % 32) / DK)
    sign = np.where(lane % DK < 32, -1.0, 1.0)
    start = (np.arange(BLOCKS) * STRETCH)[:, None] * freqs
    step = np.arange(STRETCH)[:, None] * freqs
    base = np.zeros((BLOCKS, 8, KEYS))
    base[:, 0], base[:, 1], base[:, 2] = np.cos(start), np.sin(start), sign * np.sin(start)
    turn = np.stack([np.cos(step), np.sin(step), sign * np.sin(step)])
    lg = -(0.25 + 0.25 * np.arange(4)) / (BLOCKS * STRETCH)
    pos = np.arange(STRETCH)
    decay = np.zeros((2, 208, KEYS))
    mask = np.zeros((2, 4, STRETCH, 2, STRETCH))
    gap = pos[:, None] - pos[None, :]
    for t in range(2):
        for h in range(2):
            g = lg[2 * t + h]
            decay[t, :64, h * DK : (h + 1) * DK] = np.exp((STRETCH - 1 - pos) * g)[:, None]
            decay[t, 64 + 64 * h : 128 + 64 * h] = np.exp((pos + 1) * g)[:, None]
            decay[t, 192 + 8 * h : 200 + 8 * h] = np.exp(STRETCH * g)
            for s in range(2):
                mask[t, 2 * h + s, :, s] = np.where(gap >= 0, np.exp(np.maximum(gap, 0) * g), 0)
    mask = mask.reshape(2, 4 * STRETCH, 2 * STRETCH)
    return [np.asarray(a, np.float32) for a in (base, turn, decay, mask)]


def dot(a, b):
    return jnp.dot(a, b, preferred_element_type=F32)


def layer(
    x_hbm, gain_hbm, wq_hbm, wk_hbm, wv_hbm, wg_hbm, hg_hbm, wo_hbm, init_hbm,
    base_hbm, turn_hbm, decay_hbm, mask_hbm,
    mix, mix_oth, w_own, w_oth, closing,
    x_own, x_oth, gain, w_in, hgain, init, base, turn, decay, mask,
    normed, cosine, sine, keys, wkeys, values, queries, gate, inner,
    send1, recv1, send2, incoming, csend,
    load_sem, xs_sem, xr_sem, a_send, a_recv, sem2, sem3,
):
    z, y, x, t = (lax.axis_index(a) for a in SP_TP)
    me = (z * 4 + y) * 4 + x

    piece = me // 4
    loads = [
        pltpu.make_async_copy(src, dst, load_sem.at[k])
        for k, (src, dst) in enumerate(
            (
                (x_hbm, x_own),
                (gain_hbm, gain),
                (wk_hbm, w_in.at[:, pl.ds(0, KEYS)]),
                (wv_hbm, w_in.at[:, pl.ds(KEYS, VALS)]),
                (base_hbm.at[me], base),
                (turn_hbm, turn),
                (decay_hbm.at[t], decay),
                (wq_hbm, w_in.at[:, pl.ds(KEYS + VALS, KEYS)]),
                (wg_hbm, w_in.at[:, pl.ds(2 * KEYS + VALS, VALS)]),
                (hg_hbm, hgain),
                (mask_hbm.at[t], mask),
                (init_hbm.at[piece // 2, lax.rem(piece, 2), pl.ds(TILE * lax.rem(me, 4), TILE)], init),
                (wo_hbm, w_own),
            )
        )
    ]
    partner = (z, y, x, 1 - t)
    barrier = pltpu.get_barrier_semaphore()
    for k in (1, 2, 3):
        for there in (
            (lax.rem(z + k, 4), y, x, t),
            (z, lax.rem(y + k, 4), x, t),
            (z, y, lax.rem(x + k, 4), t),
        ):
            pl.semaphore_signal(barrier, inc=1, device_id=there, device_id_type=MESH)
    pl.semaphore_signal(barrier, inc=1, device_id=partner, device_id_type=MESH)
    for copy in loads:
        copy.start()

    pl.semaphore_wait(barrier, 10)
    for k in (1, 2, 3):
        pl.semaphore_signal(sem2, inc=1, device_id=(z, lax.rem(y + k, 4), x, t), device_id_type=MESH)
    loads[0].wait()
    swap_x = pltpu.make_async_remote_copy(
        src_ref=x_own, dst_ref=x_oth, send_sem=xs_sem.at[0], recv_sem=xr_sem.at[0],
        device_id=partner, device_id_type=MESH,
    )
    swap_x.start()

    for k in range(1, 7):
        loads[k].wait()
    cosine[...] = base[0:1, :] * turn[0] - base[1:2, :] * turn[1]
    sine[...] = base[2:3, :] * turn[0] + base[0:1, :] * turn[2]

    lane = lax.broadcasted_iota(jnp.int32, (1, 1, KEYS), 2)
    low = lax.rem(lane, DK) < DK // 2
    gains = gain[...].astype(F32).reshape(1, D)

    def norm(x_ref, side):
        def rows(s, carry):
            f = x_ref[s].astype(F32)
            ms = jnp.mean(f * f, axis=-1, keepdims=True)
            normed[side, pl.ds(pl.multiple_of(s * HALF, HALF), HALF), :] = (
                f * lax.rsqrt(ms + EPS) * gains
            ).astype(BF16)
            return carry

        lax.fori_loop(0, SEQS, rows, 0)

    def rotary(p, row):
        v = p.reshape(SEQS, HALF, KEYS)
        flat = p
        other = jnp.where(
            low, pltpu.roll(flat, KEYS - 32, 1).reshape(v.shape), pltpu.roll(flat, 32, 1).reshape(v.shape)
        )
        return v * cosine[pl.ds(row, HALF), :][None] + other * sine[pl.ds(row, HALF), :][None]

    def keys_values(side, row):
        p = dot(normed[side], w_in[:, : KEYS + VALS])
        values[:, pl.ds(row, HALF), :] = p[:, KEYS:].astype(BF16).reshape(SEQS, HALF, VALS)
        k = (rotary(p[:, :KEYS].astype(BF16).astype(F32), row) * DK**-0.5).astype(BF16)
        keys[:, pl.ds(row, HALF), :] = k
        wkeys[:, pl.ds(row, HALF), :] = (k.astype(F32) * decay[pl.ds(row, HALF), :][None]).astype(BF16)

    def queries_gates(side, row):
        p = dot(normed[side], w_in[:, KEYS + VALS :])
        queries[:, pl.ds(row, HALF), :] = rotary(p[:, :KEYS].astype(BF16).astype(F32), row).astype(BF16)
        g = p[:, KEYS:].astype(BF16).astype(F32)
        gate[:, pl.ds(row, HALF), :] = jax.nn.silu(g).reshape(SEQS, HALF, VALS)

    row_own = pl.multiple_of(HALF * t, HALF)
    row_oth = pl.multiple_of(HALF * (1 - t), HALF)
    norm(x_own, 0)
    pl.semaphore_wait(sem2, 3)
    for k in (1, 2, 3):
        pl.semaphore_signal(sem3, inc=1, device_id=(lax.rem(z + k, 4), y, x, t), device_id_type=MESH)
    keys_values(0, row_own)
    swap_x.wait()
    loads[12].wait()
    swap_w = pltpu.make_async_remote_copy(
        src_ref=w_own, dst_ref=w_oth, send_sem=xs_sem.at[1], recv_sem=xr_sem.at[1],
        device_id=partner, device_id_type=MESH,
    )
    swap_w.start()
    norm(x_oth, 1)
    keys_values(1, row_oth)

    for s in range(SEQS):
        both = dot(wkeys[s].T, values[s])
        for h in range(2):
            part = both[h * DK : (h + 1) * DK, h * DV : (h + 1) * DV].astype(BF16)
            send1[pl.ds((2 * s + h) * 4, 4)] = part.reshape(4, TILE, DV)
    pl.semaphore_wait(sem3, 3)

    def to_all(source, landing, k_sem):
        zs, ys, xs = ([lax.rem(a + k, 4) for k in range(4)] for a in (z, y, x))
        for kz, ky, kx in FAR_FIRST:
            there = (zs[kz] * 4 + ys[ky]) * 4 + xs[kx]
            pltpu.make_async_remote_copy(
                src_ref=source(there), dst_ref=landing.at[me],
                send_sem=a_send.at[k_sem], recv_sem=a_recv.at[k_sem],
                device_id=(zs[kz], ys[ky], xs[kx], t), device_id_type=MESH,
            ).start()

    def await_all(buffer, sem):
        rest = buffer.at[pl.ds(0, BLOCKS - 1)]
        pltpu.make_async_copy(rest, rest, sem).wait()

    to_all(lambda there: send1.at[there], recv1, 0)
    recv1[me] = send1[me]

    for k in range(7, 12):
        loads[k].wait()
    queries_gates(0, row_own)
    queries_gates(1, row_oth)
    block_decay = decay[pl.ds(pl.multiple_of(192 + 8 * lax.rem(piece, 2), 8), 8), :]
    block_decay = jnp.concatenate([block_decay, block_decay], axis=0)
    await_all(recv1, a_recv.at[0])
    state = init[...]
    for j in range(BLOCKS):
        send2[j] = state.astype(BF16)
        state = state * block_decay + recv1[j].astype(F32)
    csend[...] = state.astype(BF16)
    to_all(lambda there: send2.at[there], incoming, 1)
    incoming[me] = send2[me]
    first = lax.broadcasted_iota(jnp.int32, (1, KEYS), 1) < DK
    for j in range(SEQS // 2):
        q = queries[2 * j : 2 * j + 2].reshape(2 * STRETCH, KEYS)
        zero = jnp.zeros_like(q)
        stacked = jnp.concatenate([jnp.where(first, q, zero), jnp.where(first, zero, q)], axis=0)
        k = keys[2 * j : 2 * j + 2].reshape(2 * STRETCH, KEYS)
        scores = lax.dot_general(stacked, k, (((1,), (1,)), ((), ())), preferred_element_type=F32)
        scores = (scores * mask[...]).astype(BF16)
        v = values[2 * j : 2 * j + 2].reshape(2 * STRETCH, VALS)
        for h in range(2):
            cols = slice(h * DV, (h + 1) * DV)
            got = dot(scores[h * 2 * STRETCH : (h + 1) * 2 * STRETCH], v[:, cols])
            inner[2 * j : 2 * j + 2, :, cols] = got.reshape(2, STRETCH, DV)

    to_all(lambda there: csend, closing, 2)
    closing[me] = csend[...]
    await_all(incoming, a_recv.at[1])

    gains_h = hgain[...].astype(F32)
    for s in range(SEQS):
        q = queries[s]
        s0 = incoming[pl.ds(8 * s, 4)].reshape(DK, DV)
        s1 = incoming[pl.ds(8 * s + 4, 4)].reshape(DK, DV)
        zero = jnp.zeros_like(s0)
        cross = dot(q, jnp.concatenate(
            [jnp.concatenate([s0, zero], axis=1), jnp.concatenate([zero, s1], axis=1)], axis=0
        ))
        for h in range(2):
            cols = slice(h * DV, (h + 1) * DV)
            kept = inner[s, :, cols] + cross[:, cols] * decay[64 + 64 * h : 128 + 64 * h, :]
            kept = kept - jnp.mean(kept, axis=-1, keepdims=True)
            spread = jnp.mean(kept * kept, axis=-1, keepdims=True)
            m = gate[s, :, cols] * (kept * lax.rsqrt(spread + EPS) * gains_h[h : h + 1, :])
            m = m.astype(BF16)
            mix[0, s, :, cols] = m[:HALF]
            mix[1, s, :, cols] = m[HALF:]
    swap_m = pltpu.make_async_remote_copy(
        src_ref=mix.at[1 - t], dst_ref=mix_oth, send_sem=xs_sem.at[2], recv_sem=xr_sem.at[2],
        device_id=partner, device_id_type=MESH,
    )
    swap_m.start()
    await_all(closing, a_recv.at[2])
    await_all(send1, a_send.at[0])
    await_all(send2, a_send.at[1])
    await_all(closing, a_send.at[2])
    swap_w.wait()
    swap_m.wait()


def project_out(mix, mix_oth, w_own, w_oth, closing, out_hbm, close_hbm, out, close, sem):
    t = lax.axis_index("tp")
    close[...] = closing[...].astype(F32).reshape(SEQS, 2, DK, DV)
    stores = [pltpu.make_async_copy(close, close_hbm, sem.at[0])]
    stores[0].start()
    for k in range(SEQS // 2):
        seqs = pl.ds(2 * k, 2)
        part = dot(mix[t, seqs].reshape(2 * HALF, VALS), w_own[...])
        part = part + dot(mix_oth[seqs].reshape(2 * HALF, VALS), w_oth[...])
        out[seqs] = part.astype(BF16).reshape(2, HALF, D)
        stores.append(pltpu.make_async_copy(out.at[seqs], out_hbm.at[seqs], sem.at[1 + k]))
        stores[-1].start()
    for store in stores:
        store.wait()


def per_device(x, norm_gain, w_query, w_key, w_value, w_gate, head_gain, w_out, initial_state):
    any_space = pl.BlockSpec(memory_space=pl.ANY)
    vmem = pltpu.VMEM
    in_vmem = pl.BlockSpec(memory_space=vmem)
    dma = pltpu.SemaphoreType.DMA
    rows = (SEQS, STRETCH)
    args = (
        x, norm_gain, w_query, w_key, w_value, w_gate, head_gain, w_out, initial_state,
        *[jnp.asarray(a) for a in tables()],
    )
    handed = pl.pallas_call(
        layer,
        out_shape=(
            vmem((2, SEQS, HALF, VALS), BF16),
            vmem((SEQS, HALF, VALS), BF16),
            vmem((VALS, D), BF16),
            vmem((VALS, D), BF16),
            vmem((BLOCKS, TILE, DV), BF16),
        ),
        in_specs=[any_space] * len(args),
        out_specs=(in_vmem,) * 5,
        scratch_shapes=[
            vmem((SEQS, HALF, D), BF16),
            vmem((SEQS, HALF, D), BF16),
            vmem((D,), BF16),
            vmem((D, 2 * (KEYS + VALS)), BF16),
            vmem((2, DV), BF16),
            vmem((TILE, DV), F32),
            vmem((8, KEYS), F32),
            vmem((3, STRETCH, KEYS), F32),
            vmem((208, KEYS), F32),
            vmem((4 * STRETCH, 2 * STRETCH), F32),
            vmem((2, SEQS * HALF, D), BF16),
            vmem((STRETCH, KEYS), F32),
            vmem((STRETCH, KEYS), F32),
            vmem(rows + (KEYS,), BF16),
            vmem(rows + (KEYS,), BF16),
            vmem(rows + (VALS,), BF16),
            vmem(rows + (KEYS,), BF16),
            vmem(rows + (VALS,), F32),
            vmem(rows + (VALS,), F32),
            vmem((BLOCKS, TILE, DV), BF16),
            vmem((BLOCKS, TILE, DV), BF16),
            vmem((BLOCKS, TILE, DV), BF16),
            vmem((BLOCKS, TILE, DV), BF16),
            vmem((TILE, DV), BF16),
            dma((13,)), dma((3,)), dma((3,)), dma((3,)), dma((3,)),
            pltpu.SemaphoreType.REGULAR, pltpu.SemaphoreType.REGULAR,
        ],
        compiler_params=pltpu.CompilerParams(collective_id=0, has_side_effects=True),
    )(*args)
    return pl.pallas_call(
        project_out,
        out_shape=(
            jax.ShapeDtypeStruct(x.shape, BF16),
            jax.ShapeDtypeStruct(initial_state.shape, F32),
        ),
        in_specs=[in_vmem] * 5,
        out_specs=(any_space, any_space),
        scratch_shapes=[
            vmem((SEQS, HALF, D), BF16),
            vmem((SEQS, 2, DK, DV), F32),
            dma((1 + SEQS // 2,)),
        ],
    )(*[pltpu.with_memory_space_constraint(a, vmem) for a in handed])


def solution(mesh):
    split = Mesh(mesh.devices.reshape(4, 4, 4, mesh.shape["tp"]), SP_TP)
    placed = (
        P(None, SP_TP, None),
        P(),
        P(None, "tp"),
        P(None, "tp"),
        P(None, "tp"),
        P(None, "tp"),
        P("tp", None),
        P("tp", None),
        P(None, "tp", None, None),
    )
    return jax.shard_map(
        per_device,
        mesh=split,
        in_specs=placed,
        out_specs=(P(None, SP_TP, None), P(None, "tp", None, None)),
        check_vma=False,
    )
```
